32 devices in a mesh: fs: 8 (over z, y), tp: 4 (over x, core).
Axes of the slice: x: 2, y: 2, z: 4, core: 2. Of those that a mesh axis runs over, the one named last changes fastest.
Arguments:
- later_gate: bfloat16 [5120, 5632], P('fs', 'tp'), may hold values from -6 to 6
- later_up: bfloat16 [5120, 5632], P('fs', 'tp'), may hold values from -6 to 6
- early_gate: bfloat16 [5120, 5632], P('fs', 'tp'), may hold values from -6 to 6
- early_up: bfloat16 [5120, 5632], P('fs', 'tp'), may hold values from -6 to 6
- early_cotangent: bfloat16 [5120, 2048], P(('fs', 'tp')), may hold values from -6 to 6
- down_weight: bfloat16 [5632, 2048], P('tp', 'fs'), may hold values from -0.078125 to 0.078125
- grad_running: float32 [5632, 2048], P('tp', 'fs'), may hold values from -224 to 224
Outputs:
- mixed: bfloat16 [5120, 2048], P(('fs', 'tp'))
- gate_grad: bfloat16 [5120, 5632], P('fs', 'tp')
- up_grad: bfloat16 [5120, 5632], P('fs', 'tp')
- grad_total: float32 [5632, 2048], P('tp', 'fs')
The draws below stay inside these ranges and needn't reach their ends.
All inputs are finite; a program needn't handle non-finite values.
Results may differ from the reference program's by a relative error of at most 0.009.
Values may be sent and summed in bfloat16 or wider, within the bound.
A program may use at most 128 MiB of HBM per device.

```python
import jax
import jax.numpy as jnp

D = 2048
FF = 5632
TOKENS = 5120
N_TP = 4


def raised(entries, own_key, source, target, shards_of, factor):
    owner, partner = [(jnp.arange(entries.shape[dim]) // (entries.shape[dim] // shards_of)).reshape([-1 if axis == dim else 1 for axis in range(entries.ndim)]) for dim in (source, target)]
    chosen = jax.random.permutation(own_key, shards_of)[partner]
    strong = (owner == chosen) | (owner == (partner + shards_of // 2) % shards_of)
    return jnp.where(strong, factor * entries, entries)


def steps_of(rng, extent, pieces, least, top_value):
    factor_of, own = 1.0, jax.random.fold_in(rng, 6)
    for axis_at, shards_of in pieces:
        steps = jnp.exp(jax.random.uniform(jax.random.fold_in(own, axis_at), (shards_of,), jnp.float32, least / len(pieces), top_value / len(pieces)))
        factor_of = factor_of * jnp.repeat(steps, extent[axis_at] // shards_of).reshape([-1 if axis == axis_at else 1 for axis in range(len(extent))])
    return factor_of


def centred(rng, shape, width, reach, shards=(), kind=jnp.bfloat16):
    values = jax.random.normal(rng, shape, jnp.float32) * width
    if len(shards) > 0:
        values = steps_of(rng, shape, shards, -0.22, 0.18) * values
    return jnp.clip(values, min=-reach, max=reach).astype(kind)


def bell_draw_with(own_key, shape, spread, most, cuts, heavy, dtype=jnp.bfloat16):
    drawn = spread * jax.random.normal(own_key, shape, jnp.float32)
    if cuts:
        drawn = drawn * steps_of(own_key, shape, cuts, -0.22, 0.18)
    return jnp.clip(raised(drawn, jax.random.fold_in(own_key, 3), *heavy), -most, most).astype(dtype)


def setup_inputs(seed: int = 0) -> dict:
    key_list = jax.random.split(jax.random.key(seed), 8)
    return {
        "later_gate": centred(key_list[0], (TOKENS, FF), 1.0, 6.0, ((0, 8), (1, 4))),
        "later_up": centred(key_list[1], (TOKENS, FF), 1.0, 6.0, ((0, 8), (1, 4))),
        "early_gate": centred(key_list[2], (TOKENS, FF), 1.0, 6.0, ((0, 8), (1, 4))),
        "early_up": centred(key_list[3], (TOKENS, FF), 1.0, 6.0, ((0, 8), (1, 4))),
        "early_cotangent": bell_draw_with(key_list[4], (TOKENS, D), 1.0, 6.0, ((0, 32),), (0, 1, 32, 2.75)),
        "down_weight": centred(key_list[5], (FF, D), FF ** -0.5, 0.078125, ((0, 4), (1, 8))),
        "grad_running": centred(key_list[6], (FF, D), (0.5 * TOKENS ** 0.5), 224.0, ((0, 4), (1, 8)), jnp.float32),
    }


def reference(later_gate, later_up, early_gate, early_up, early_cotangent, down_weight, grad_running):
    later_hidden = (jax.nn.silu(later_gate.astype(jnp.float32)) * later_up.astype(jnp.float32)).astype(jnp.bfloat16)
    block = FF // N_TP
    total = jnp.zeros((later_hidden.shape[0], D), jnp.float32)
    for index in range(N_TP):
        part = jnp.dot(later_hidden[:, index * block:(index + 1) * block], down_weight[index * block:(index + 1) * block], preferred_element_type=jnp.float32)
        total = total + part.astype(jnp.bfloat16).astype(jnp.float32)
    mixed = total.astype(jnp.bfloat16)
    gate_value = early_gate.astype(jnp.float32)
    up_value = early_up.astype(jnp.float32)
    sigma = jax.nn.sigmoid(gate_value)
    early_hidden = (gate_value * sigma * up_value).astype(jnp.bfloat16)
    hidden_cot = jnp.dot(early_cotangent, down_weight.T, preferred_element_type=jnp.float32)
    gate_grad = (hidden_cot * up_value * sigma * (1.0 + gate_value * (1.0 - sigma))).astype(jnp.bfloat16)
    up_grad = (hidden_cot * gate_value * sigma).astype(jnp.bfloat16)
    grad_total = grad_running + jnp.dot(early_hidden.T, early_cotangent, preferred_element_type=jnp.float32)
    return (mixed, gate_grad, up_grad, grad_total)
```

```python
import functools

import jax
import jax.numpy as jnp
from jax import lax
from jax.experimental import pallas as pl
from jax.experimental.pallas import tpu as pltpu
from jax.sharding import PartitionSpec as P

PAIR = 2
F32, BF16 = jnp.float32, jnp.bfloat16


def by_collectives(
    later_gate, later_up, early_gate, early_up, early_cotangent, down_weight, grad_running
):
    later_hidden = (
        jax.nn.silu(later_gate.astype(F32)) * later_up.astype(F32)
    ).astype(BF16)
    gate_value = early_gate.astype(F32)
    up_value = early_up.astype(F32)
    sigma = jax.nn.sigmoid(gate_value)
    early_hidden = (gate_value * sigma * up_value).astype(BF16)
    cot_rows = lax.all_gather(early_cotangent, "tp", axis=0, tiled=True)
    whole = lax.all_gather(down_weight, "fs", axis=1, tiled=True)
    mixed = lax.psum_scatter(
        jnp.dot(later_hidden, whole, preferred_element_type=F32).astype(BF16),
        "tp",
        scatter_dimension=0,
        tiled=True,
    )
    hidden_cot = lax.dot_general(
        cot_rows, whole, (((1,), (1,)), ((), ())), preferred_element_type=F32
    )
    gate_grad = (hidden_cot * up_value * sigma * (1.0 + gate_value * (1.0 - sigma))).astype(BF16)
    up_grad = (hidden_cot * gate_value * sigma).astype(BF16)
    summed = lax.psum_scatter(
        lax.dot_general(
            cot_rows, early_hidden, (((0,), (0,)), ((), ())), preferred_element_type=F32
        ),
        "fs",
        scatter_dimension=0,
        tiled=True,
    )
    return (mixed, gate_grad, up_grad, grad_running + summed.T)


def kernel(
    fs, n,
    lg_ref, lu_ref, eg_ref, eu_ref, cot_ref, w_ref, gr_ref,
    mixed_ref, gg_ref, ug_ref, gt_ref,
    lg, lu, eg, eu, run, W, C, Cp, He, Hl, Gs, Gr, own_g, Ms, Mr, hc, mixed,
    loc, wup_s, wdn_s, wy_s, w_r, c_s, c_r, cy_s, cy_r, cp_s, cp_r, h_s, h_r, g_s, g_r, m_s, m_r,
):
    Z = fs // PAIR
    T, K = lg.shape
    B = W.shape[2]
    R = T // n
    me_f, me = lax.axis_index("fs"), lax.axis_index("tp")
    z, y = me_f // PAIR, me_f % PAIR
    buddy = {"fs": z * PAIR + 1 - y}

    def remote(src, dst, ss, rs, to):
        return pltpu.make_async_remote_copy(
            src_ref=src, dst_ref=dst, send_sem=ss, recv_sem=rs,
            device_id=to, device_id_type=pl.DeviceIdType.MESH,
        )

    def block(f):
        return pl.ds(pl.multiple_of(f * B, B), B)

    def rows(t):
        return pl.ds(pl.multiple_of(t * R, R), R)

    others_z = [lax.rem(z + k, Z) for k in range(1, Z)]
    others_t = [lax.rem(me + k, n) for k in range(1, n)]

    loads = [
        pltpu.make_async_copy(src, dst, loc.at[i])
        for i, (src, dst) in enumerate((
            (w_ref, W.at[me_f]), (cot_ref, C.at[rows(me), :]), (eg_ref, eg), (eu_ref, eu),
            (lg_ref, lg), (lu_ref, lu), (gr_ref, run),
        ))
    ]
    for copy in loads:
        copy.start()

    barrier = pltpu.get_barrier_semaphore()
    for to in [buddy] + [{"fs": k * PAIR + y} for k in others_z] + [{"tp": t} for t in others_t]:
        pl.semaphore_signal(barrier, inc=1, device_id=to, device_id_type=pl.DeviceIdType.MESH)
    pl.semaphore_wait(barrier, 1 + len(others_z) + len(others_t))

    def up(zz):
        f = zz * PAIR + y
        return remote(W.at[f], W.at[f], wup_s.at[zz], w_r.at[f], {"fs": (z + 1) * PAIR + y})

    def down(zz):
        f = zz * PAIR + y
        return remote(W.at[f], W.at[f], wdn_s.at[zz], w_r.at[f], {"fs": (z - 1) * PAIR + y})

    def across(zz):
        f = zz * PAIR + y
        return remote(W.at[f], W.at[f], wy_s.at[zz], w_r.at[f], buddy)

    def got_w(f):
        remote(W.at[f], W.at[f], wy_s.at[0], w_r.at[f], buddy).wait_recv()

    loads[0].wait()

    @pl.when(z < Z - 1)
    def _():
        up(z).start()

    @pl.when(z > 0)
    def _():
        down(z).start()

    loads[1].wait()
    cy = [
        remote(
            C.at[rows(me), block(k * PAIR + 1 - y)], Cp.at[rows(me), pl.ds(k * B, B)],
            cy_s.at[k], cy_r.at[k], buddy,
        )
        for k in range(Z)
    ]
    for copy in cy:
        copy.start()
    for t in others_t:
        remote(C.at[rows(me), :], C.at[rows(me), :], c_s.at[t], c_r.at[me], {"tp": t}).start()

    step = 32 if T % 32 == 0 else R

    def hidden(g_ref, u_ref, out):
        @pl.loop(0, T // step)
        def _(i):
            at = pl.ds(pl.multiple_of(i * step, step), step)
            g = g_ref[at, :].astype(F32)
            out[at, :] = (g * jax.nn.sigmoid(g) * u_ref[at, :].astype(F32)).astype(BF16)

    loads[2].wait()
    loads[3].wait()
    hidden(eg, eu, He.at[0])
    swap = remote(He.at[0], He.at[1], h_s.at[0], h_r.at[0], buddy)
    swap.start()

    for copy in cy:
        copy.wait_recv()
    for t in others_t:
        remote(Cp.at[rows(me), :], Cp.at[rows(me), :], cp_s.at[t], cp_r.at[me], {"tp": t}).start()

    loads[4].wait()
    loads[5].wait()
    hidden(lg, lu, Hl)

    def m_copy(f, t):
        return remote(
            Ms.at[rows(t), block(f)], Mr.at[me, :, block(f)],
            m_s.at[f * n + t], m_r.at[f * n + me], {"tp": t},
        )

    def mix(f):
        @pl.loop(0, n)
        def _(t):
            part = jnp.dot(Hl[rows(t), :], W[f], preferred_element_type=F32)
            Ms[rows(t), block(f)] = part.astype(BF16)

        for t in others_t:
            m_copy(f, t).start()

    cuts = [(a, min(a + 512, K)) for a in range(0, K, 512)]

    def back(f, first):
        @pl.loop(0, n)
        def _(t):
            c = C[rows(t), block(f)]
            for a, b in cuts:
                term = lax.dot_general(
                    c, W[f, a:b, :], (((1,), (1,)), ((), ())), preferred_element_type=F32
                )
                hc[rows(t), a:b] = term if first else hc[rows(t), a:b] + term

    def in_order(body):
        @pl.loop(0, 2 * Z - 1)
        def _(c):
            d = (c + 1) // 2
            zz = jnp.where(c % 2 == 1, z - d, z + d)

            @pl.when((zz >= 0) & (zz < Z))
            def _():
                body(c, zz)

    def relay(c, zz):
        @pl.when(c > 0)
        def _():
            got_w(zz * PAIR + y)

        @pl.when((c > 0) & (zz < z) & (z < Z - 1))
        def _():
            up(zz).start()

        @pl.when((c > 0) & (zz > z) & (z > 0))
        def _():
            down(zz).start()

        across(zz).start()
        mix(zz * PAIR + y)

    in_order(relay)

    for t in others_t:
        remote(C.at[rows(t), :], C.at[rows(t), :], c_s.at[t], c_r.at[t], {"tp": t}).wait_recv()
        remote(Cp.at[rows(t), :], Cp.at[rows(t), :], cp_s.at[t], cp_r.at[t], {"tp": t}).wait_recv()
    swap.wait_recv()
    over_rows = (((0,), (0,)), ((), ()))

    @pl.loop(0, K // 128)
    def _(i):
        at = pl.ds(pl.multiple_of(i * 128, 128), 128)
        mine, theirs = He[0, :, at], He[1, :, at]
        for k in range(Z):
            zz = lax.rem(z + k, Z)
            term = lax.dot_general(
                mine, C[:, block(zz * PAIR + y)], over_rows, preferred_element_type=F32
            ) + lax.dot_general(theirs, Cp[:, block(zz)], over_rows, preferred_element_type=F32)
            if k == 0:
                own_g[at, :] = term
            else:
                Gs[zz, at, :] = term.astype(BF16)

    def g_copy(zz):
        return remote(Gs.at[zz], Gr.at[z], g_s.at[zz], g_r.at[z], {"fs": zz * PAIR + y})

    for zz in others_z:
        g_copy(zz).start()

    back(z * PAIR + y, True)
    in_order(lambda c, zz: pl.when(c > 0)(lambda: back(zz * PAIR + y, False)))

    def partner(c, zz):
        f = zz * PAIR + 1 - y
        got_w(f)
        mix(f)
        back(f, False)

    in_order(partner)

    outs = []

    @pl.loop(0, T // step)
    def _(i):
        at = pl.ds(pl.multiple_of(i * step, step), step)
        g, u, h = eg[at, :].astype(F32), eu[at, :].astype(F32), hc[at, :]
        s = jax.nn.sigmoid(g)
        lg[at, :] = (h * u * s * (1.0 + g * (1.0 - s))).astype(BF16)
        lu[at, :] = (h * g * s).astype(BF16)

    outs.append(pltpu.make_async_copy(lg, gg_ref, loc.at[7]))
    outs.append(pltpu.make_async_copy(lu, ug_ref, loc.at[8]))
    for copy in outs:
        copy.start()

    for zz in others_z:
        remote(Gs.at[zz], Gr.at[zz], g_s.at[zz], g_r.at[zz], buddy).wait_recv()
    loads[6].wait()

    @pl.loop(0, K // 128)
    def _(i):
        at = pl.ds(pl.multiple_of(i * 128, 128), 128)
        total = own_g[at, :]
        for zz in others_z:
            total = total + Gr[zz, at, :].astype(F32)
        own_g[at, :] = run[at, :] + total

    outs.append(pltpu.make_async_copy(own_g, gt_ref, loc.at[9]))
    outs[-1].start()

    @pl.loop(0, fs)
    def _(f):
        for t in others_t:
            remote(
                Ms.at[rows(t), block(f)], Mr.at[t, :, block(f)],
                m_s.at[f * n + t], m_r.at[f * n + t], {"tp": t},
            ).wait_recv()
        total = Ms[rows(me), block(f)].astype(F32)
        for t in others_t:
            total = total + Mr[t, :, block(f)].astype(F32)
        mixed[:, block(f)] = total.astype(BF16)

    outs.append(pltpu.make_async_copy(mixed, mixed_ref, loc.at[10]))
    outs[-1].start()

    def sent(c, zz):
        @pl.when((zz <= z) & (z < Z - 1))
        def _():
            up(zz).wait_send()

        @pl.when((zz >= z) & (z > 0))
        def _():
            down(zz).wait_send()

        across(zz).wait_send()

    in_order(sent)
    for copy in cy:
        copy.wait_send()
    for t in others_t:
        remote(C.at[rows(me), :], C.at[rows(me), :], c_s.at[t], c_r.at[me], {"tp": t}).wait_send()
        remote(Cp.at[rows(me), :], Cp.at[rows(me), :], cp_s.at[t], cp_r.at[me], {"tp": t}).wait_send()
    swap.wait_send()
    for zz in others_z:
        g_copy(zz).wait_send()

    @pl.loop(0, fs)
    def _(f):
        for t in others_t:
            m_copy(f, t).wait_send()

    for copy in outs:
        copy.wait()


def by_kernel(fs, n, *args):
    later_gate, cot, weight = args[0], args[4], args[5]
    T, K = later_gate.shape
    R, D = cot.shape
    B = weight.shape[1]
    Z = fs // PAIR
    sem = pltpu.SemaphoreType.DMA
    anywhere = pl.BlockSpec(memory_space=pl.ANY)
    return pl.pallas_call(
        functools.partial(kernel, fs, n),
        out_shape=(
            jax.ShapeDtypeStruct((R, D), BF16),
            jax.ShapeDtypeStruct((T, K), BF16),
            jax.ShapeDtypeStruct((T, K), BF16),
            jax.ShapeDtypeStruct((K, B), F32),
        ),
        in_specs=[anywhere] * 7,
        out_specs=(anywhere,) * 4,
        scratch_shapes=[
            pltpu.VMEM((T, K), BF16), pltpu.VMEM((T, K), BF16),
            pltpu.VMEM((T, K), BF16), pltpu.VMEM((T, K), BF16),
            pltpu.VMEM((K, B), F32),
            pltpu.VMEM((fs, K, B), BF16),
            pltpu.VMEM((T, D), BF16),
            pltpu.VMEM((T, Z * B), BF16),
            pltpu.VMEM((2, T, K), BF16),
            pltpu.VMEM((T, K), BF16),
            pltpu.VMEM((Z, K, B), BF16), pltpu.VMEM((Z, K, B), BF16),
            pltpu.VMEM((K, B), F32),
            pltpu.VMEM((T, D), BF16),
            pltpu.VMEM((n, R, D), BF16),
            pltpu.VMEM((T, K), F32),
            pltpu.VMEM((R, D), BF16),
            sem((11,)),
            sem((Z,)), sem((Z,)), sem((Z,)), sem((fs,)),
            sem((n,)), sem((n,)), sem((Z,)), sem((Z,)), sem((n,)), sem((n,)),
            sem((1,)), sem((1,)), sem((Z,)), sem((Z,)),
            sem((fs * n,)), sem((fs * n,)),
        ],
        compiler_params=pltpu.CompilerParams(
            collective_id=0, has_side_effects=True, vmem_limit_bytes=62 * 2**20
        ),
    )(*args)


def solution(mesh):
    fs, n = mesh.shape["fs"], mesh.shape["tp"]

    def on_device(*args):
        T, K = args[0].shape
        B = args[5].shape[1]
        if fs % PAIR == 0 and fs >= 4 and B % 128 == 0 and K % 128 == 0 and (T // n) % 32 == 0:
            return by_kernel(fs, n, *args)
        return by_collectives(*args)

    placed = (
        P("fs", "tp"),
        P("fs", "tp"),
        P("fs", "tp"),
        P("fs", "tp"),
        P(("fs", "tp"), None),
        P("tp", "fs"),
        P("tp", "fs"),
    )
    return jax.shard_map(
        on_device,
        mesh=mesh,
        in_specs=placed,
        out_specs=(P(("fs", "tp"), None), P("fs", "tp"), P("fs", "tp"), P("tp", "fs")),
        check_vma=False,
    )
```

```python
import functools

import jax
import jax.numpy as jnp
from jax import lax
from jax.experimental import pallas as pl
from jax.experimental.pallas import tpu as pltpu
from jax.sharding import PartitionSpec as P

PAIR = 2
F32, BF16 = jnp.float32, jnp.bfloat16


def by_collectives(
    later_gate, later_up, early_gate, early_up, early_cotangent, down_weight, grad_running
):
    later_hidden = (
        jax.nn.silu(later_gate.astype(F32)) * later_up.astype(F32)
    ).astype(BF16)
    gate_value = early_gate.astype(F32)
    up_value = early_up.astype(F32)
    sigma = jax.nn.sigmoid(gate_value)
    early_hidden = (gate_value * sigma * up_value).astype(BF16)
    cot_rows = lax.all_gather(early_cotangent, "tp", axis=0, tiled=True)
    whole = lax.all_gather(down_weight, "fs", axis=1, tiled=True)
    mixed = lax.psum_scatter(
        jnp.dot(later_hidden, whole, preferred_element_type=F32).astype(BF16),
        "tp",
        scatter_dimension=0,
        tiled=True,
    )
    hidden_cot = lax.dot_general(
        cot_rows, whole, (((1,), (1,)), ((), ())), preferred_element_type=F32
    )
    gate_grad = (hidden_cot * up_value * sigma * (1.0 + gate_value * (1.0 - sigma))).astype(BF16)
    up_grad = (hidden_cot * gate_value * sigma).astype(BF16)
    summed = lax.psum_scatter(
        lax.dot_general(
            cot_rows, early_hidden, (((0,), (0,)), ((), ())), preferred_element_type=F32
        ),
        "fs",
        scatter_dimension=0,
        tiled=True,
    )
    return (mixed, gate_grad, up_grad, grad_running + summed.T)


def parts_of(K):
    size = -(-(K // 128) // 4) * 128
    return [(a, min(a + size, K)) for a in range(0, K, size)]


def kernel(
    fs, n,
    lg_ref, lu_ref, eg_ref, eu_ref, cot_ref, w_ref, gr_ref,
    mixed_ref, gg_ref, ug_ref, gt_ref,
    lg, lu, eg, eu, run, W, C, Cp, He, Hl, Gs, Gr, own_g, Ms, Mr, hc, mixed,
    loc, wup_s, wdn_s, wy_s, w_r, c_s, c_r, cy_s, cy_r, cp_s, cp_r, h_s, h_r, g_s, g_r, m_s, m_r,
    wb_s, wb_r, wbu_s, wbd_s,
):
    Z = fs // PAIR
    T, K = lg.shape
    B = W.shape[2]
    R = T // n
    early = max(K * 3 // 22 // 64, 1) * 64
    me_f, me = lax.axis_index("fs"), lax.axis_index("tp")
    z, y = me_f // PAIR, me_f % PAIR
    buddy = {"fs": z * PAIR + 1 - y}

    def remote(src, dst, ss, rs, to):
        return pltpu.make_async_remote_copy(
            src_ref=src, dst_ref=dst, send_sem=ss, recv_sem=rs,
            device_id=to, device_id_type=pl.DeviceIdType.MESH,
        )

    def block(f):
        return pl.ds(pl.multiple_of(f * B, B), B)

    def rows(t):
        return pl.ds(pl.multiple_of(t * R, R), R)

    others_z = [lax.rem(z + k, Z) for k in range(1, Z)]
    others_t = [lax.rem(me + k, n) for k in range(1, n)]

    loads = [
        pltpu.make_async_copy(src, dst, loc.at[i])
        for i, (src, dst) in enumerate((
            (w_ref, W.at[me_f]), (cot_ref, C.at[rows(me), :]), (eg_ref, eg), (eu_ref, eu),
            (lg_ref, lg), (lu_ref, lu), (gr_ref, run),
        ))
    ]
    for copy in loads:
        copy.start()

    barrier = pltpu.get_barrier_semaphore()
    for to in [buddy] + [{"fs": k * PAIR + y} for k in others_z] + [{"tp": t} for t in others_t]:
        pl.semaphore_signal(barrier, inc=1, device_id=to, device_id_type=pl.DeviceIdType.MESH)
    pl.semaphore_wait(barrier, 1 + len(others_z) + len(others_t))

    def up(zz):
        f = zz * PAIR + y
        return remote(W.at[f], W.at[f], wup_s.at[zz], w_r.at[f], {"fs": (z + 1) * PAIR + y})

    def down(zz):
        f = zz * PAIR + y
        return remote(W.at[f], W.at[f], wdn_s.at[zz], w_r.at[f], {"fs": (z - 1) * PAIR + y})

    def across(zz, source=y):
        f = zz * PAIR + source
        part = W.at[f, early:, :]
        return remote(part, part, wy_s.at[zz], w_r.at[f], buddy)

    def first_across():
        part = W.at[me_f, :early, :]
        return remote(part, part, wb_s.at[0], wb_r.at[z], buddy)

    def first_up(zz):
        part = W.at[zz * PAIR + 1 - y, :early, :]
        return remote(part, part, wbu_s.at[zz], wb_r.at[zz], {"fs": (z + 1) * PAIR + y})

    def first_down(zz):
        part = W.at[zz * PAIR + 1 - y, :early, :]
        return remote(part, part, wbd_s.at[zz], wb_r.at[zz], {"fs": (z - 1) * PAIR + y})

    def got_w(f):
        remote(W.at[f], W.at[f], wy_s.at[0], w_r.at[f], buddy).wait_recv()

    loads[0].wait()

    @pl.when(z < Z - 1)
    def _():
        up(z).start()

    @pl.when(z > 0)
    def _():
        down(z).start()

    first_across().start()
    loads[1].wait()
    cy = [
        remote(
            C.at[rows(me), block(k * PAIR + 1 - y)], Cp.at[rows(me), pl.ds(k * B, B)],
            cy_s.at[k], cy_r.at[k], buddy,
        )
        for k in range(Z)
    ]
    for copy in cy:
        copy.start()

    def c_copy(t, f, source):
        part = C.at[rows(source), block(f)]
        return remote(part, part, c_s.at[t * fs + f], c_r.at[source * fs + f], {"tp": t})

    def c_send(side):
        for k in range(Z):
            for t in others_t:
                c_copy(t, k * PAIR + side, me).start()

    def c_wait(side):
        for k in range(Z):
            for t in others_t:
                c_copy(t, k * PAIR + side, t).wait_recv()

    c_send(y)
    step = 32 if T % 32 == 0 else R

    def hidden(g_ref, u_ref, out, a, b):
        @pl.loop(0, T // step)
        def _(i):
            at = pl.ds(pl.multiple_of(i * step, step), step)
            g = g_ref[at, a:b].astype(F32)
            out[at, a:b] = (g * jax.nn.sigmoid(g) * u_ref[at, a:b].astype(F32)).astype(BF16)

    loads[2].wait()
    loads[3].wait()
    swaps = []
    for q, (a, b) in enumerate(parts_of(K)):
        hidden(eg, eu, He.at[0], a, b)
        swaps.append(
            remote(He.at[0, :, a:b], He.at[1, :, a:b], h_s.at[q], h_r.at[q], buddy)
        )
        swaps[-1].start()

    for copy in cy:
        copy.wait_recv()
    for t in others_t:
        remote(Cp.at[rows(me), :], Cp.at[rows(me), :], cp_s.at[t], cp_r.at[me], {"tp": t}).start()
    c_send(1 - y)

    loads[4].wait()
    loads[5].wait()
    hidden(lg, lu, Hl, 0, K)

    def m_copy(f, t):
        return remote(
            Ms.at[rows(t), block(f)], Mr.at[me, :, block(f)],
            m_s.at[f * n + t], m_r.at[f * n + me], {"tp": t},
        )

    def mix(f):
        @pl.loop(0, n)
        def _(t):
            part = jnp.dot(Hl[rows(t), :], W[f], preferred_element_type=F32)
            Ms[rows(t), block(f)] = part.astype(BF16)

        for t in others_t:
            m_copy(f, t).start()

    cuts = [(a, min(a + 512, K)) for a in range(0, K, 512)]

    def back(f, first):
        @pl.loop(0, n)
        def _(t):
            c = C[rows(t), block(f)]
            for a, b in cuts:
                term = lax.dot_general(
                    c, W[f, a:b, :], (((1,), (1,)), ((), ())), preferred_element_type=F32
                )
                hc[rows(t), a:b] = term if first else hc[rows(t), a:b] + term

    def in_order(body, first=0, end=2 * Z - 1):
        @pl.loop(first, end)
        def _(c):
            d = (c + 1) // 2
            zz = jnp.where(c % 2 == 1, z - d, z + d)

            @pl.when((zz >= 0) & (zz < Z))
            def _():
                body(c, zz)

    def relay(c, zz):
        @pl.when(c > 0)
        def _():
            got_w(zz * PAIR + y)

        @pl.when((c > 0) & (zz < z) & (z < Z - 1))
        def _():
            up(zz).start()

        @pl.when((c > 0) & (zz > z) & (z > 0))
        def _():
            down(zz).start()

        part = W.at[zz * PAIR + 1 - y, :early, :]
        remote(part, part, wb_s.at[0], wb_r.at[zz], buddy).wait_recv()

        @pl.when((zz <= z) & (z < Z - 1))
        def _():
            first_up(zz).start()

        @pl.when((zz >= z) & (z > 0))
        def _():
            first_down(zz).start()

        across(zz).start()
        mix(zz * PAIR + y)

    over_rows = (((0,), (0,)), ((), ()))

    def g_copy(q, zz, source):
        a, b = parts_of(K)[q]
        return remote(
            Gs.at[zz, a:b, :], Gr.at[source, a:b, :],
            g_s.at[q * Z + zz], g_r.at[q * Z + source], {"fs": zz * PAIR + y},
        )

    def terms(q):
        swaps[q].wait_recv()
        a, b = parts_of(K)[q]

        @pl.loop(a // 128, b // 128)
        def _(i):
            at = pl.ds(pl.multiple_of(i * 128, 128), 128)
            mine, theirs = He[0, :, at], He[1, :, at]
            for k in range(Z):
                zz = lax.rem(z + k, Z)
                term = lax.dot_general(
                    mine, C[:, block(zz * PAIR + y)], over_rows, preferred_element_type=F32
                ) + lax.dot_general(theirs, Cp[:, block(zz)], over_rows, preferred_element_type=F32)
                if k == 0:
                    own_g[at, :] = term
                else:
                    Gs[zz, at, :] = term.astype(BF16)

        for zz in others_z:
            g_copy(q, zz, z).start()

    parts = len(parts_of(K))
    near = min(5, 2 * Z - 1)
    in_order(relay, 0, near)
    c_wait(y)
    for t in others_t:
        remote(Cp.at[rows(t), :], Cp.at[rows(t), :], cp_s.at[t], cp_r.at[t], {"tp": t}).wait_recv()
    for q in range(parts // 2):
        terms(q)
    in_order(relay, near)
    for q in range(parts // 2, parts):
        terms(q)
    c_wait(1 - y)

    back(z * PAIR + y, True)
    in_order(lambda c, zz: pl.when(c > 0)(lambda: back(zz * PAIR + y, False)))

    def partner(c, zz):
        f = zz * PAIR + 1 - y
        across(zz, 1 - y).wait_recv()
        mix(f)
        back(f, False)

    in_order(partner)

    outs = []

    for t in range(n):
        @pl.loop(t * R // step, (t + 1) * R // step)
        def _(i):
            at = pl.ds(pl.multiple_of(i * step, step), step)
            g, u, h = eg[at, :].astype(F32), eu[at, :].astype(F32), hc[at, :]
            s = jax.nn.sigmoid(g)
            lg[at, :] = (h * u * s * (1.0 + g * (1.0 - s))).astype(BF16)
            lu[at, :] = (h * g * s).astype(BF16)

        at = pl.ds(t * R, R)
        outs.append(pltpu.make_async_copy(lg.at[at, :], gg_ref.at[at, :], loc.at[9 + 2 * t]))
        outs.append(pltpu.make_async_copy(lu.at[at, :], ug_ref.at[at, :], loc.at[10 + 2 * t]))
        outs[-2].start()
        outs[-1].start()

    for q in range(parts):
        for zz in others_z:
            g_copy(q, zz, zz).wait_recv()
    loads[6].wait()

    @pl.loop(0, K // 128)
    def _(i):
        at = pl.ds(pl.multiple_of(i * 128, 128), 128)
        total = own_g[at, :]
        for zz in others_z:
            total = total + Gr[zz, at, :].astype(F32)
        own_g[at, :] = run[at, :] + total

    outs.append(pltpu.make_async_copy(own_g, gt_ref, loc.at[7]))
    outs[-1].start()

    @pl.loop(0, fs)
    def _(f):
        for t in others_t:
            remote(
                Ms.at[rows(t), block(f)], Mr.at[t, :, block(f)],
                m_s.at[f * n + t], m_r.at[f * n + t], {"tp": t},
            ).wait_recv()
        total = Ms[rows(me), block(f)].astype(F32)
        for t in others_t:
            total = total + Mr[t, :, block(f)].astype(F32)
        mixed[:, block(f)] = total.astype(BF16)

    outs.append(pltpu.make_async_copy(mixed, mixed_ref, loc.at[8]))
    outs[-1].start()

    def sent(c, zz):
        @pl.when((zz <= z) & (z < Z - 1))
        def _():
            up(zz).wait_send()
            first_up(zz).wait_send()

        @pl.when((zz >= z) & (z > 0))
        def _():
            down(zz).wait_send()
            first_down(zz).wait_send()

        across(zz).wait_send()

    in_order(sent)
    first_across().wait_send()
    for copy in cy:
        copy.wait_send()
    for t in others_t:
        for f in range(fs):
            c_copy(t, f, me).wait_send()
        remote(Cp.at[rows(me), :], Cp.at[rows(me), :], cp_s.at[t], cp_r.at[me], {"tp": t}).wait_send()
    for copy in swaps:
        copy.wait_send()
    for q in range(parts):
        for zz in others_z:
            g_copy(q, zz, z).wait_send()

    @pl.loop(0, fs)
    def _(f):
        for t in others_t:
            m_copy(f, t).wait_send()

    for copy in outs:
        copy.wait()


def by_kernel(fs, n, *args):
    later_gate, cot, weight = args[0], args[4], args[5]
    T, K = later_gate.shape
    R, D = cot.shape
    B = weight.shape[1]
    Z = fs // PAIR
    parts = len(parts_of(K))
    sem = pltpu.SemaphoreType.DMA
    anywhere = pl.BlockSpec(memory_space=pl.ANY)
    return pl.pallas_call(
        functools.partial(kernel, fs, n),
        out_shape=(
            jax.ShapeDtypeStruct((R, D), BF16),
            jax.ShapeDtypeStruct((T, K), BF16),
            jax.ShapeDtypeStruct((T, K), BF16),
            jax.ShapeDtypeStruct((K, B), F32),
        ),
        in_specs=[anywhere] * 7,
        out_specs=(anywhere,) * 4,
        scratch_shapes=[
            pltpu.VMEM((T, K), BF16), pltpu.VMEM((T, K), BF16),
            pltpu.VMEM((T, K), BF16), pltpu.VMEM((T, K), BF16),
            pltpu.VMEM((K, B), F32),
            pltpu.VMEM((fs, K, B), BF16),
            pltpu.VMEM((T, D), BF16),
            pltpu.VMEM((T, Z * B), BF16),
            pltpu.VMEM((2, T, K), BF16),
            pltpu.VMEM((T, K), BF16),
            pltpu.VMEM((Z, K, B), BF16), pltpu.VMEM((Z, K, B), BF16),
            pltpu.VMEM((K, B), F32),
            pltpu.VMEM((T, D), BF16),
            pltpu.VMEM((n, R, D), BF16),
            pltpu.VMEM((T, K), F32),
            pltpu.VMEM((R, D), BF16),
            sem((9 + 2 * n,)),
            sem((Z,)), sem((Z,)), sem((Z,)), sem((fs,)),
            sem((n * fs,)), sem((n * fs,)), sem((Z,)), sem((Z,)), sem((n,)), sem((n,)),
            sem((parts,)), sem((parts,)), sem((parts * Z,)), sem((parts * Z,)),
            sem((fs * n,)), sem((fs * n,)),
            sem((1,)), sem((Z,)), sem((Z,)), sem((Z,)),
        ],
        compiler_params=pltpu.CompilerParams(
            collective_id=0, has_side_effects=True, vmem_limit_bytes=62 * 2**20
        ),
    )(*args)


def solution(mesh):
    fs, n = mesh.shape["fs"], mesh.shape["tp"]

    def on_device(*args):
        T, K = args[0].shape
        B = args[5].shape[1]
        if fs % PAIR == 0 and fs >= 4 and B % 128 == 0 and K % 128 == 0 and (T // n) % 32 == 0:
            return by_kernel(fs, n, *args)
        return by_collectives(*args)

    placed = (
        P("fs", "tp"),
        P("fs", "tp"),
        P("fs", "tp"),
        P("fs", "tp"),
        P(("fs", "tp"), None),
        P("tp", "fs"),
        P("tp", "fs"),
    )
    return jax.shard_map(
        on_device,
        mesh=mesh,
        in_specs=placed,
        out_specs=(P(("fs", "tp"), None), P("fs", "tp"), P("fs", "tp"), P("tp", "fs")),
        check_vma=False,
    )
```
